32 devices in a mesh: grp: 2 (over y), fs: 4 (over z), tp: 4 (over x, core).
Axes of the slice: x: 2, y: 2, z: 4, core: 2. Of those that a mesh axis runs over, the one named last changes fastest.
Arguments:
- tokens: bfloat16 [8192, 2048], P(('grp', 'fs'), 'tp'), parts along dimension 0, may hold values from -50 to 50
- mix_gain: float32 [2048], replicated, may hold values from 0.1 to 1.9
- value_proj: bfloat16 [2048, 1024], P('fs', 'tp'), may hold values from -0.125 to 0.125
- gate_proj: bfloat16 [2048, 1024], P('fs', 'tp'), may hold values from -0.125 to 0.125
- conv_taps: float32 [31, 1024], P(None, 'tp'), may hold values from -1 to 1
- chan_gain: float32 [1024], replicated, may hold values from 0.1 to 1.9
- chan_shift: float32 [1024], replicated, may hold values from -3 to 3
- mix_out: bfloat16 [1024, 2048], P('fs', 'tp'), may hold values from -0.1875 to 0.1875
- mlp_gain: float32 [2048], replicated, may hold values from 0.1 to 1.9
- mlp_gate: bfloat16 [2048, 5632], P('fs', 'tp'), may hold values from -0.125 to 0.125
- mlp_up: bfloat16 [2048, 5632], P('fs', 'tp'), may hold values from -0.125 to 0.125
- gate_taps: float32 [3, 5632], P(None, 'tp'), may hold values from -3.5 to 3.5
- up_taps: float32 [3, 5632], P(None, 'tp'), may hold values from -3.5 to 3.5
- mlp_down: bfloat16 [5632, 2048], P('tp', 'fs'), may hold values from -0.078125 to 0.078125
- final_gain: float32 [2048], P('tp'), may hold values from 0.1 to 1.9
Outputs:
- layer_out: bfloat16 [8192, 2048], P(('grp', 'fs'), 'tp'), parts along dimension 0
The draws below stay inside these ranges and needn't reach their ends.
There are 2 independent parts, one for each index of `grp`. The reference program is written for one: setup_inputs(seed, part) draws one part's arguments, and reference() takes and returns one part's arrays. A program takes and returns all parts, laid end to end along the dimension named above; an argument that names none is the same for every part. Nothing has to cross between parts.
All inputs are finite; a program needn't handle non-finite values.
Results may differ from the reference program's by a relative error of at most 0.0095.
Values may be sent and summed in bfloat16 or wider, within the bound.
A program may use at most 128 MiB of HBM per device.

```python
import math
import jax
import jax.numpy as jnp
from jax import lax

D = 2048
CA = 1024
FF = 5632
KW = 31
FKW = 3
TOK_DEV = 1024
TOKENS = 4096
FF_BLOCK = 1408
N_TP = 4


def draw_tokens(key, part):
    base_key = jax.random.fold_in(key, 7)
    key_rows, key_cols, key_vals = jax.random.split(base_key, 3)
    lowest = 0.3
    values = jnp.clip(jax.random.normal(key_vals, (TOKENS, D), jnp.float32), -4.0, 4.0)
    row_scale = jnp.exp(jax.random.uniform(key_rows, (TOKENS, 1), jnp.float32, math.log(lowest), math.log(3.0)))
    ramp = jnp.exp(jnp.linspace(math.log(0.4), math.log(2.5), D, dtype=jnp.float32))[None, :]
    col_scale = ramp * jnp.exp(jax.random.uniform(key_cols, (1, D), jnp.float32, -0.5, 0.5))
    return (values * row_scale * col_scale).astype(jnp.bfloat16)


def steps_of(key, dims, pieces, least, largest):
    level = 1.0
    for dim, blocks in pieces:
        draws = jax.random.uniform(jax.random.fold_in(jax.random.fold_in(key, 6), dim), (blocks,), jnp.float32, least / len(pieces), largest / len(pieces))
        level = level * jnp.repeat(jnp.exp(draws), dims[dim] // blocks).reshape((-1,) + (1,) * (len(dims) - 1 - dim))
    return level


def normal_values(own_key, extent, scale, reach, cuts=(), kind=jnp.bfloat16):
    array = scale * jax.random.normal(own_key, extent, jnp.float32)
    if cuts:
        array = array * steps_of(own_key, extent, cuts, -0.22, 0.18)
    return jnp.clip(array, -reach, reach).astype(kind)


def setup_inputs(seed: int = 0, part: int = 0) -> dict:
    splits = jax.random.split(jax.random.key(seed), 16)
    part_keys = jax.random.split(jax.random.fold_in(splits[15], part), 16)
    return {
        "tokens": draw_tokens(jax.random.fold_in(jax.random.fold_in(splits[15], part), 71), part),
        "mix_gain": jnp.clip(1.0 + 0.18 * jax.random.normal(splits[1], (D,), jnp.float32), 0.1, 1.9),
        "value_proj": normal_values(splits[2], (D, CA), D ** -0.5, 0.125, ((0, 4), (1, 4))),
        "gate_proj": normal_values(splits[3], (D, CA), D ** -0.5, 0.125, ((0, 4), (1, 4))),
        "conv_taps": normal_values(splits[4], (KW, CA), KW ** -0.5, 1.0, ((1, 4),), jnp.float32),
        "chan_gain": jnp.clip(1.0 + 0.18 * jax.random.normal(splits[5], (CA,), jnp.float32), 0.1, 1.9),
        "chan_shift": normal_values(splits[6], (CA,), 0.5, 3.0, (), jnp.float32),
        "mix_out": normal_values(splits[7], (CA, D), CA ** -0.5, 0.1875, ((0, 4), (1, 4))),
        "mlp_gain": jnp.clip(1.0 + 0.18 * jax.random.normal(splits[8], (D,), jnp.float32), 0.1, 1.9),
        "mlp_gate": normal_values(splits[9], (D, FF), D ** -0.5, 0.125, ((0, 4), (1, 4))),
        "mlp_up": normal_values(splits[10], (D, FF), D ** -0.5, 0.125, ((0, 4), (1, 4))),
        "gate_taps": normal_values(splits[11], (FKW, FF), FKW ** -0.5, 3.5, ((1, 4),), jnp.float32),
        "up_taps": normal_values(splits[12], (FKW, FF), FKW ** -0.5, 3.5, ((1, 4),), jnp.float32),
        "mlp_down": normal_values(splits[13], (FF, D), FF ** -0.5, 0.078125, ((0, 4), (1, 4))),
        "final_gain": jnp.clip(1.0 + 0.18 * jax.random.normal(splits[14], (D,), jnp.float32), 0.1, 1.9),
    }


def rms_scale(values, gain):
    return values * lax.rsqrt(lax.optimization_barrier(jnp.mean(values * values, axis=-1, keepdims=True)) + 1e-06) * gain

def along_sequences(values, taps, seq_len):
    width = taps.shape[0]
    half = (width - 1) // 2
    channels = values.shape[1]
    grouped = values.reshape(-1, seq_len, channels)
    padded = jnp.pad(grouped, ((0, 0), (half, width - 1 - half), (0, 0)))
    total = jnp.zeros_like(grouped)
    for offset in range(width):
        total = total + taps[offset] * padded[:, offset:offset + seq_len]
    return total.reshape(values.shape)

def reference(tokens, mix_gain, value_proj, gate_proj, conv_taps, chan_gain, chan_shift, mix_out, mlp_gain, mlp_gate, mlp_up, gate_taps, up_taps, mlp_down, final_gain):
    base = tokens.astype(jnp.float32)
    normed = rms_scale(base, mix_gain).astype(jnp.bfloat16)
    value = jnp.dot(normed, value_proj, preferred_element_type=jnp.float32)
    gate = jnp.dot(normed, gate_proj, preferred_element_type=jnp.float32)
    glu = value * jax.nn.sigmoid(gate)
    conv_out = along_sequences(glu, conv_taps, TOK_DEV).astype(jnp.bfloat16)
    conv_wide = conv_out.astype(jnp.float32)
    mean = lax.optimization_barrier(jnp.mean(conv_wide, axis=-1, keepdims=True))
    var = lax.optimization_barrier(jnp.mean(conv_wide * conv_wide, axis=-1, keepdims=True)) - mean * mean
    chan_norm = (conv_wide - mean) * lax.rsqrt(var + 1e-05) * chan_gain + chan_shift
    hidden_mix = jax.nn.silu(chan_norm).astype(jnp.bfloat16)
    mixed = (base + jnp.dot(hidden_mix, mix_out, preferred_element_type=jnp.float32)).astype(jnp.bfloat16)
    mixed_wide = mixed.astype(jnp.float32)
    normed_two = rms_scale(mixed_wide, mlp_gain).astype(jnp.bfloat16)
    gate_conv = along_sequences(jnp.dot(normed_two, mlp_gate, preferred_element_type=jnp.float32), gate_taps, TOK_DEV)
    up_conv = along_sequences(jnp.dot(normed_two, mlp_up, preferred_element_type=jnp.float32), up_taps, TOK_DEV)
    hidden_mlp = (jax.nn.silu(gate_conv) * up_conv).astype(jnp.bfloat16)
    mlp_out = jnp.zeros((tokens.shape[0], D), jnp.float32)
    for block in range(N_TP):
        lower = block * FF_BLOCK
        partial_sum = jnp.dot(hidden_mlp[:, lower:lower + FF_BLOCK], mlp_down[lower:lower + FF_BLOCK], preferred_element_type=jnp.float32)
        rounded = lax.optimization_barrier(partial_sum.astype(jnp.bfloat16))
        mlp_out = mlp_out + rounded.astype(jnp.float32)
    summed = mixed_wide + mlp_out
    return rms_scale(summed, final_gain).astype(jnp.bfloat16)
```

```python
import jax
import jax.numpy as jnp
from jax import lax
from jax.sharding import PartitionSpec as P


DOWN_PIECES = 2
SUM_CHUNKS = 2


def along_sequence(values, taps):
    width = taps.shape[0]
    half = (width - 1) // 2
    length = values.shape[0]
    padded = jnp.pad(values, ((half, width - 1 - half), (0, 0)))
    total = jnp.zeros_like(values)
    for offset in range(width):
        total = total + taps[offset] * padded[offset : offset + length]
    return total


def put(whole, piece, index):
    return lax.dynamic_update_slice_in_dim(whole, piece[None], index, 0)


def take(parts, index, axis=0):
    return lax.dynamic_index_in_dim(parts, index, axis, keepdims=False)


def shifted(value, axis, shift):
    size = lax.axis_size(axis)
    return lax.ppermute(value, axis, [(i, (i + shift) % size) for i in range(size)])


def swapped(value, mask):
    size = lax.axis_size("tp")
    return lax.ppermute(value, "tp", [(i, i ^ mask) for i in range(size)])


def masks_of_size(size):
    assert size & (size - 1) == 0
    return [1 << bit for bit in range(size.bit_length() - 1)]


def masks_of(axis):
    return masks_of_size(lax.axis_size(axis))


def gathered_features(own):
    me = lax.axis_index("tp")
    whole = put(jnp.zeros((lax.axis_size("tp"),) + own.shape, own.dtype), own, me)
    held = [(0, own)]
    for mask in reversed(masks_of("tp")):
        for code, block in held[:]:
            held.append((code ^ mask, swapped(block, mask)))
    for code, block in held[1:]:
        whole = put(whole, block, me ^ code)
    return whole


def scattered_sum(blocks, first, count):
    me = lax.axis_index("tp")
    k, columns = blocks.shape[1], blocks.shape[3]

    def block(index):
        piece = lax.dynamic_slice(blocks, (index, 0, first, 0), (1, k, count, columns))
        return piece.reshape(k * count, columns)

    keep, send = None, None
    for mask in masks_of("tp"):
        bit = (me // mask) % 2
        if keep is None:
            half = range(blocks.shape[0] // 2)
            send = [block(2 * i + 1 - bit) for i in half]
            keep = [block(2 * i + bit) for i in half]
        else:
            pairs = list(zip(sums[0::2], sums[1::2]))
            send = [jnp.where(bit == 1, low, high).astype(jnp.bfloat16) for low, high in pairs]
            keep = [jnp.where(bit == 1, high, low) for low, high in pairs]
        sums = [
            own.astype(jnp.float32) + swapped(other, mask).astype(jnp.float32)
            for own, other in zip(keep, send)
        ]
    return sums[0].reshape(k, count, columns)


def parts_of(shard, pieces=1):
    count = lax.axis_size("grp") * pieces
    return shard.reshape(count, shard.shape[0] // count, shard.shape[1])


def shards_by_arrival(shard, pieces=1):
    groups = lax.axis_size("grp")
    group = lax.axis_index("grp")
    parts = parts_of(shard, pieces)
    arrived = [None]
    moving = [take(parts, group * pieces + i) for i in range(pieces)]
    for _ in range(1, lax.axis_size("fs")):
        got = []
        for i in range(pieces):
            moving[i] = shifted(moving[i], "fs", 1)
            got.append((group * pieces + i, moving[i]))
            for jump in range(1, groups):
                other = shifted(moving[i], "grp", jump)
                got.append(((group - jump) % groups * pieces + i, other))
        arrived.append(got)
    return arrived


def gathered_rows(shard):
    size = lax.axis_size("fs")
    groups = lax.axis_size("grp")
    me = lax.axis_index("fs")
    parts = parts_of(shard)
    whole = jnp.zeros((size * groups,) + parts.shape[1:], shard.dtype)
    whole = lax.dynamic_update_slice_in_dim(whole, parts, me * groups, 0)
    for step, got in enumerate(shards_by_arrival(shard)):
        for part, piece in got or ():
            whole = put(whole, piece, (me - step) % size * groups + part)
    return whole.reshape(size * shard.shape[0], shard.shape[1])


def over_blocks(blocks, weight):
    weight = weight.reshape(blocks.shape[0], blocks.shape[2], weight.shape[1])
    return jnp.einsum("btk,bkn->tn", blocks, weight, preferred_element_type=jnp.float32)


def normed_blocks(blocks, gain):
    values = blocks.astype(jnp.float32)
    mean = jnp.mean(values * values, axis=(0, 2), keepdims=True)
    gain = gain.reshape(blocks.shape[0], 1, blocks.shape[2])
    return (values * lax.rsqrt(mean + 1e-06) * gain).astype(jnp.bfloat16)


def local(
    tokens,
    mix_gain,
    value_proj,
    gate_proj,
    conv_taps,
    chan_gain,
    chan_shift,
    mix_out,
    mlp_gain,
    mlp_gate,
    mlp_up,
    gate_taps,
    up_taps,
    mlp_down,
    final_gain,
):
    width_tp = lax.axis_size("tp")
    size_fs = lax.axis_size("fs")
    me_fs = lax.axis_index("fs")
    rows = tokens.shape[0]
    whole = gathered_features(tokens)
    full_in = gathered_rows(jnp.concatenate([value_proj, gate_proj], axis=1))
    full_mix = gathered_rows(mix_out)
    full_gate = gathered_rows(mlp_gate)
    full_up = gathered_rows(mlp_up)
    down_shards = shards_by_arrival(mlp_down, DOWN_PIECES)
    both = over_blocks(normed_blocks(whole, mix_gain), full_in)
    own_channels = value_proj.shape[1]
    glu = both[:, :own_channels] * jax.nn.sigmoid(both[:, own_channels:])
    conv_out = along_sequence(glu, conv_taps).astype(jnp.bfloat16)
    all_channels = own_channels * width_tp
    conv_wide = conv_out.astype(jnp.float32)
    totals = lax.psum(
        (
            jnp.sum(conv_wide, axis=-1, keepdims=True),
            jnp.sum(conv_wide * conv_wide, axis=-1, keepdims=True),
        ),
        "tp",
    )
    mean = totals[0] / all_channels
    var = totals[1] / all_channels - mean * mean
    offset_ch = lax.axis_index("tp") * own_channels
    gain_own = lax.dynamic_slice_in_dim(chan_gain, offset_ch, own_channels, 0)
    shift_own = lax.dynamic_slice_in_dim(chan_shift, offset_ch, own_channels, 0)
    chan_norm = (conv_wide - mean) * lax.rsqrt(var + 1e-05) * gain_own + shift_own
    hidden_own = jax.nn.silu(chan_norm).astype(jnp.bfloat16)
    hidden_mix = gathered_features(hidden_own)
    mixer_result = over_blocks(hidden_mix, full_mix)
    mixed = (tokens.astype(jnp.float32) + mixer_result).astype(jnp.bfloat16)
    normed_two = normed_blocks(gathered_features(mixed), mlp_gain)
    gate_conv = along_sequence(over_blocks(normed_two, full_gate), gate_taps)
    up_conv = along_sequence(over_blocks(normed_two, full_up), up_taps)
    hidden_mlp = (jax.nn.silu(gate_conv) * up_conv).astype(jnp.bfloat16)
    hidden_mlp = lax.optimization_barrier(hidden_mlp)
    partial_terms = jnp.zeros((size_fs, rows, mlp_down.shape[1]), jnp.bfloat16)
    for step, got in enumerate(down_shards):
        weight = mlp_down
        if got:
            weight = jnp.zeros(parts_of(mlp_down, DOWN_PIECES).shape, mlp_down.dtype)
            for part, piece in got:
                weight = put(weight, piece, part)
            weight = weight.reshape(mlp_down.shape)
        columns = jnp.dot(hidden_mlp, weight, preferred_element_type=jnp.float32)
        partial_terms = put(partial_terms, columns.astype(jnp.bfloat16), (me_fs - step) % size_fs)
    per_owner = size_fs // width_tp
    assert per_owner * width_tp == size_fs
    partial_terms = partial_terms.reshape(width_tp, per_owner, rows, mlp_down.shape[1])
    chunk = rows // SUM_CHUNKS
    sums = [
        scattered_sum(partial_terms, i * chunk, chunk) for i in range(SUM_CHUNKS)
    ]
    mlp_out = jnp.moveaxis(jnp.concatenate(sums, axis=1), 0, 1).reshape(mixed.shape)
    summed = mixed.astype(jnp.float32) + mlp_out
    squares = lax.psum(jnp.sum(summed * summed, axis=-1, keepdims=True), "tp")
    all_features = summed.shape[1] * width_tp
    layer_out = summed * lax.rsqrt(squares / all_features + 1e-06) * final_gain
    return layer_out.astype(jnp.bfloat16)


def solution(mesh):
    return jax.shard_map(
        local,
        mesh=mesh,
        in_specs=(
            P(("grp", "fs"), "tp"),
            P(),
            P("fs", "tp"),
            P("fs", "tp"),
            P(None, "tp"),
            P(),
            P(),
            P("fs", "tp"),
            P(),
            P("fs", "tp"),
            P("fs", "tp"),
            P(None, "tp"),
            P(None, "tp"),
            P("tp", "fs"),
            P("tp"),
        ),
        out_specs=P(("grp", "fs"), "tp"),
        check_vma=False,
    )
```
